32 devices in a mesh: sp: 8 (over z, x), tp: 4 (over y, core).
Axes of the slice: x: 2, y: 2, z: 4, core: 2. Of those that a mesh axis runs over, the one named last changes fastest.
Arguments:
- query_rows: bfloat16 [4096, 1024], P('sp', 'tp'), may hold values from -6 to 6
- key_rows: bfloat16 [4096, 1024], P('sp', 'tp'), may hold values from -6 to 6
- value_rows: bfloat16 [4096, 2048], P('sp', 'tp'), may hold values from -6 to 6
- out_gate_pre: bfloat16 [4096, 2048], P('sp', 'tp'), may hold values from -8 to 8
- input_gate_pre: float32 [4, 4096], P('tp', 'sp'), may hold values from -8 to 8
- forget_gate_pre: float32 [4, 4096], P('tp', 'sp'), may hold values from -26 to 26
- residual: bfloat16 [4096, 2048], P(('sp', 'tp')), may hold values from -6 to 6
- out_proj: bfloat16 [2048, 2048], P('tp'), may hold values from -0.125 to 0.125
- mix_gain: float32 [2048], replicated, may hold values from 0.1 to 1.9
- pre_gain: float32 [2048], replicated, may hold values from 0.1 to 1.9
- gate_proj: bfloat16 [2048, 3072], P('sp', 'tp'), may hold values from -0.125 to 0.125
- value_proj: bfloat16 [2048, 3072], P('sp', 'tp'), may hold values from -0.125 to 0.125
- gate_kernel: float32 [3, 3072], P(None, 'tp'), may hold values from -3.5 to 3.5
- value_kernel: float32 [3, 3072], P(None, 'tp'), may hold values from -3.5 to 3.5
- down_proj: bfloat16 [2048, 3072], P('sp', 'tp'), may hold values from -0.109375 to 0.109375
- post_gain: float32 [2048], replicated, may hold values from 0.1 to 1.9
Outputs:
- result: bfloat16 [4096, 2048], P(('sp', 'tp'))
The draws below stay inside these ranges and needn't reach their ends.
All inputs are finite; a program needn't handle non-finite values.
Results may differ from the reference program's by a relative error of at most 0.017.
Values may be sent and summed in bfloat16 or wider, within the bound.
No kernel may reach another device: no remote copies, remote signals or barrier semaphores. Data moves between devices by JAX's collectives and lax.ppermute only.
A program may use at most 128 MiB of HBM per device.

```python
import math
import jax
import jax.numpy as jnp
from jax import lax

D = 2048
HEADS = 4
QK = 256
HV = 512
FF = 3072
BLOCK = 64
CONV = 3
TOK_DEV = 512
SEQUENCE_TOKENS = 4096
N_TP = 4


def draw_forget_gate_pre(key, part):
    sequence_lanes = jax.random.split(jax.random.fold_in(key, 7301), 6)
    order = jax.random.permutation(sequence_lanes[0], HEADS)
    slow_count = HEADS // 2
    sluggish_decay = (order < slow_count)[:, None]
    spans = SEQUENCE_TOKENS // TOK_DEV
    factor = jnp.exp(jax.random.uniform(sequence_lanes[1], (HEADS, spans), jnp.float32, math.log(0.15), math.log(0.5)))
    factor = jnp.repeat(factor, TOK_DEV, axis=1)
    slow_rate = factor * (math.log(10.0) / SEQUENCE_TOKENS)
    fast_rate = jnp.exp(-jax.random.uniform(sequence_lanes[2], (HEADS, 1), jnp.float32, math.log(8.0), math.log(40.0)))
    rate = jnp.where(sluggish_decay, slow_rate, fast_rate)
    noise = 0.7 * jax.random.normal(sequence_lanes[3], (HEADS, SEQUENCE_TOKENS), jnp.float32)
    magnitude_value = -jnp.log(rate) + noise
    spike_locations = jax.random.randint(sequence_lanes[4], (4,), 0, SEQUENCE_TOKENS)
    spiked_entries = jnp.any(jnp.arange(SEQUENCE_TOKENS)[None, :] == spike_locations[:, None], axis=0)[None, :]
    retained_entries = jax.random.uniform(sequence_lanes[5], (HEADS, SEQUENCE_TOKENS), jnp.float32, 0.5, 0.8)
    spike_height = jnp.log(retained_entries / (1.0 - retained_entries))
    magnitude_value = jnp.where(spiked_entries & sluggish_decay, spike_height, magnitude_value)
    magnitude_value = jnp.clip(magnitude_value, -14.0, 14.0)
    ratio = magnitude_value / 15.0
    return 7.5 * jnp.log((1.0 + ratio) / (1.0 - ratio))


def steps_of(rng, extent, cuts, least, high):
    loudness = 1.0
    for dim, parts in cuts:
        draws = jax.random.uniform(jax.random.fold_in(jax.random.fold_in(rng, 6), dim), (parts,), jnp.float32, least / len(cuts), high / len(cuts))
        loudness = loudness * jnp.repeat(jnp.exp(draws), extent[dim] // parts).reshape((-1,) + (1,) * (len(extent) - 1 - dim))
    return loudness


def scatter_about(rng, extent, deviation, reach, pieces=(), kind=jnp.bfloat16):
    drawn = jax.random.normal(rng, extent, jnp.float32) * deviation
    if len(pieces) > 0:
        drawn = steps_of(rng, extent, pieces, -0.22, 0.18) * drawn
    return jnp.clip(drawn, min=-reach, max=reach).astype(kind)


def setup_inputs(seed: int = 0) -> dict:
    splits = jax.random.split(jax.random.key(seed), 17)
    query_rows = scatter_about(splits[0], (SEQUENCE_TOKENS, HEADS * QK), 1.0, 6.0, ((0, 8), (1, 4)))
    key_rows = scatter_about(splits[1], (SEQUENCE_TOKENS, HEADS * QK), 1.0, 6.0, ((0, 8), (1, 4)))
    value_rows = scatter_about(splits[2], (SEQUENCE_TOKENS, HEADS * HV), 1.0, 6.0, ((0, 8), (1, 4)))
    out_gate_pre = scatter_about(splits[3], (SEQUENCE_TOKENS, HEADS * HV), 1.5, 8.0, ((0, 8), (1, 4)))
    input_gate_pre = scatter_about(splits[4], (HEADS, SEQUENCE_TOKENS), 2.0, 8.0, ((0, 4), (1, 8)), jnp.float32)
    forget_gate_pre = draw_forget_gate_pre(jax.random.fold_in(splits[16], 71), 0)
    residual = scatter_about(splits[6], (SEQUENCE_TOKENS, D), 1.0, 6.0, ((0, 32),))
    out_proj = scatter_about(splits[7], (HEADS * HV, D), (HEADS * HV) ** -0.5, 0.125, ((0, 4),))
    mix_gain = jnp.clip(1.0 + 0.18 * jax.random.normal(splits[8], (D,), jnp.float32), 0.1, 1.9)
    pre_gain = jnp.clip(1.0 + 0.18 * jax.random.normal(splits[9], (D,), jnp.float32), 0.1, 1.9)
    gate_proj = scatter_about(splits[10], (D, FF), D ** -0.5, 0.125, ((0, 8), (1, 4)))
    value_proj = scatter_about(splits[11], (D, FF), D ** -0.5, 0.125, ((0, 8), (1, 4)))
    gate_kernel = scatter_about(splits[12], (CONV, FF), CONV ** -0.5, 3.5, ((1, 4),), jnp.float32)
    value_kernel = scatter_about(splits[13], (CONV, FF), CONV ** -0.5, 3.5, ((1, 4),), jnp.float32)
    down_proj = scatter_about(splits[14], (D, FF), FF ** -0.5, 0.109375, ((0, 8), (1, 4)))
    post_gain = jnp.clip(1.0 + 0.18 * jax.random.normal(splits[15], (D,), jnp.float32), 0.1, 1.9)
    return {"query_rows": query_rows, "key_rows": key_rows, "value_rows": value_rows, "out_gate_pre": out_gate_pre, "input_gate_pre": input_gate_pre, "forget_gate_pre": forget_gate_pre, "residual": residual, "out_proj": out_proj, "mix_gain": mix_gain, "pre_gain": pre_gain, "gate_proj": gate_proj, "value_proj": value_proj, "gate_kernel": gate_kernel, "value_kernel": value_kernel, "down_proj": down_proj, "post_gain": post_gain}


gate_cap = 15.0
epsilon = 1e-06
highest = lax.Precision.HIGHEST

def softcap(values):
    return gate_cap * jnp.tanh(values / gate_cap)

def normalize(values, gains):
    return values * lax.rsqrt(lax.optimization_barrier(jnp.mean(values * values, axis=-1, keepdims=True)) + epsilon) * gains

def barrier_round(values):
    rounded = lax.optimization_barrier(values.astype(jnp.bfloat16))
    return rounded.astype(jnp.float32)

def head_cells(inputs):
    queries, key_heads, value_heads, log_input, log_forget = inputs
    nblocks = SEQUENCE_TOKENS // BLOCK
    causal = jnp.tril(jnp.ones((BLOCK, BLOCK), dtype=bool))

    def advance(carried_state, block_inputs):
        memory, normer, stabilizer = carried_state
        query_blk, key_blk, value_blk, input_blk, forget_blk = block_inputs
        running = jnp.cumsum(forget_blk)
        block_total = running[-1]
        log_weights = jnp.where(causal, running[:, None] - running[None, :] + input_blk[None, :], -jnp.inf)
        carried = running + stabilizer
        row_max = jnp.maximum(carried, lax.optimization_barrier(jnp.max(log_weights, axis=1)))
        inner_weights = jnp.exp(log_weights - row_max[:, None])
        outer_weights = jnp.exp(carried - row_max)
        scores = jnp.dot(query_blk, key_blk.T, precision=highest) * inner_weights
        numerator = outer_weights[:, None] * jnp.dot(query_blk, memory, precision=highest) + jnp.dot(scores, value_blk, precision=highest)
        denominator = outer_weights * jnp.dot(query_blk, normer, precision=highest) + lax.optimization_barrier(jnp.sum(scores, axis=1))
        cell_rows = numerator / jnp.maximum(jnp.abs(denominator), jnp.exp(-row_max))[:, None]
        lead_logs = block_total - running + input_blk
        new_stabilizer = jnp.maximum(block_total + stabilizer, jnp.max(lead_logs))
        lead_weights = jnp.exp(lead_logs - new_stabilizer)
        decay_factor = jnp.exp(block_total + stabilizer - new_stabilizer)
        weighted = key_blk * lead_weights[:, None]
        memory = decay_factor * memory + jnp.dot(weighted.T, value_blk, precision=highest)
        normer = decay_factor * normer + lax.optimization_barrier(jnp.sum(weighted, axis=0))
        return ((memory, normer, new_stabilizer), cell_rows)
    initial = (jnp.zeros((QK, HV), jnp.float32), jnp.zeros((QK,), jnp.float32), jnp.zeros((), jnp.float32))
    stacked = (queries.reshape(nblocks, BLOCK, QK), key_heads.reshape(nblocks, BLOCK, QK), value_heads.reshape(nblocks, BLOCK, HV), log_input.reshape(nblocks, BLOCK), log_forget.reshape(nblocks, BLOCK))
    ignored, outputs = lax.scan(advance, initial, stacked)
    return outputs.reshape(SEQUENCE_TOKENS, HV)

def grouped_sum(left, right, right_axis):
    group_width = left.shape[1] // N_TP
    summed = jnp.zeros((left.shape[0], right.shape[1 - right_axis]), jnp.float32)
    for group_index in range(N_TP):
        left_part = left[:, group_index * group_width:(group_index + 1) * group_width]
        right_part = lax.slice_in_dim(right, group_index * group_width, (group_index + 1) * group_width, axis=right_axis)
        partial_sum = lax.dot_general(left_part, right_part, (((1,), (right_axis,)), ((), ())), preferred_element_type=jnp.float32)
        summed = summed + barrier_round(partial_sum)
    return summed.astype(jnp.bfloat16)

def depthwise(up_rows, kernel):
    length = up_rows.shape[0]
    padded = jnp.pad(up_rows.astype(jnp.float32), ((CONV - 1, 0), (0, 0)))
    summed = kernel[0] * padded[0:length]
    for offset in range(1, CONV):
        summed = summed + kernel[offset] * padded[offset:offset + length]
    return summed

def reference(query_rows, key_rows, value_rows, out_gate_pre, input_gate_pre, forget_gate_pre, residual, out_proj, mix_gain, pre_gain, gate_proj, value_proj, gate_kernel, value_kernel, down_proj, post_gain):
    query_scale = QK ** (-0.5)
    queries = query_rows.astype(jnp.float32).reshape(SEQUENCE_TOKENS, HEADS, QK).transpose(1, 0, 2) * query_scale
    key_heads = key_rows.astype(jnp.float32).reshape(SEQUENCE_TOKENS, HEADS, QK).transpose(1, 0, 2)
    value_heads = value_rows.astype(jnp.float32).reshape(SEQUENCE_TOKENS, HEADS, HV).transpose(1, 0, 2)
    log_input = softcap(input_gate_pre)
    log_forget = jax.nn.log_sigmoid(softcap(forget_gate_pre))
    cell_rows = lax.map(head_cells, (queries, key_heads, value_heads, log_input, log_forget))
    cell_rows = cell_rows.transpose(1, 0, 2).reshape(SEQUENCE_TOKENS, HEADS * HV)
    gated = (cell_rows * jax.nn.sigmoid(out_gate_pre.astype(jnp.float32))).astype(jnp.bfloat16)
    mixed = grouped_sum(gated, out_proj, 0)
    stream = (residual.astype(jnp.float32) + normalize(mixed.astype(jnp.float32), mix_gain)).astype(jnp.bfloat16)
    normed = normalize(stream.astype(jnp.float32), pre_gain).astype(jnp.bfloat16)
    up_gate = jnp.dot(normed, gate_proj, preferred_element_type=jnp.float32).astype(jnp.bfloat16)
    up_value = jnp.dot(normed, value_proj, preferred_element_type=jnp.float32).astype(jnp.bfloat16)
    hidden = (jax.nn.silu(depthwise(up_gate, gate_kernel)) * depthwise(up_value, value_kernel)).astype(jnp.bfloat16)
    ffn = grouped_sum(hidden, down_proj, 1)
    return (stream.astype(jnp.float32) + normalize(ffn.astype(jnp.float32), post_gain)).astype(jnp.bfloat16)
```

```python
import functools

import jax
import jax.numpy as jnp
from jax import lax
from jax.experimental import pallas as pl
from jax.experimental.pallas import tpu as pltpu
from jax.sharding import PartitionSpec as P

CONV = 3
PAD = 16
gate_cap = 15.0
epsilon = 1e-06
far_below = -1e30
highest = lax.Precision.HIGHEST
f32 = jnp.float32
bf16 = jnp.bfloat16


SMEM = pl.BlockSpec(memory_space=pltpu.SMEM)
VMEM = pl.BlockSpec(memory_space=pltpu.VMEM)
HBM = pl.BlockSpec(memory_space=pltpu.HBM)


def call(kernel, out, name, args, scratch=(), specs=None):
    specs = specs or [SMEM if i == 0 else VMEM for i in range(len(args))]
    many = isinstance(out[0][0], tuple)
    return pl.pallas_call(
        kernel,
        out_shape=tuple(jax.ShapeDtypeStruct(*o) for o in out) if many else jax.ShapeDtypeStruct(*out),
        in_specs=specs,
        out_specs=tuple(VMEM for _ in out) if many else VMEM,
        scratch_shapes=list(scratch),
        name=name,
    )(*args)


def softcap(values):
    return gate_cap * jnp.tanh(values / gate_cap)


def log_gates(ig, fg):
    log_input = softcap(ig)
    capped = softcap(fg)
    log_forget = jnp.minimum(capped, 0.0) - jnp.log1p(jnp.exp(-jnp.abs(capped)))
    rows = ig.shape[1]
    upper = lax.broadcasted_iota(jnp.int32, (rows, rows), 0) <= lax.broadcasted_iota(
        jnp.int32, (rows, rows), 1
    )
    running = lax.dot_general(
        jnp.broadcast_to(log_forget, (8, rows)),
        upper.astype(f32),
        (((1,), (0,)), ((), ())),
        precision=highest,
        preferred_element_type=f32,
    )[:1]
    return log_input, running


def column(row):
    return jnp.broadcast_to(row, (128, row.shape[1])).T[:, :1]


def encode(memory, normer, total, peak):
    qk, hv = memory.shape
    side = jnp.concatenate(
        (
            normer,
            jnp.broadcast_to(total, (1, (hv - qk) // 2)),
            jnp.broadcast_to(peak, (1, (hv - qk) // 2)),
        ),
        axis=1,
    )
    high = side.astype(bf16).astype(f32)
    middle = (side - high).astype(bf16).astype(f32)
    low = (side - high - middle).astype(bf16).astype(f32)
    tail = jnp.concatenate((high, middle, low, jnp.zeros((13, hv), f32)), axis=0)
    return memory.astype(bf16), tail.astype(bf16)


def store_state(ref, h, state):
    memory, tail = encode(*state)
    qk = memory.shape[0]
    ref[h, :qk, :] = memory
    ref[h, qk:, :] = tail


def load_state(ref, h):
    qk = ref.shape[1] - 16
    hv = ref.shape[2]
    tail = ref[h, qk:, :].astype(f32)
    side = tail[0:1] + tail[1:2] + tail[2:3]
    half = (hv - qk) // 2
    return (
        ref[h, :qk, :].astype(f32),
        side[:, :qk],
        side[:, qk : qk + 1],
        side[:, qk + half : qk + half + 1],
    )


def combine(previous, following):
    prev_memory, prev_normer, prev_total, prev_peak = previous
    next_memory, next_normer, next_total, next_peak = following
    peak = jnp.maximum(next_total + prev_peak, next_peak)
    prev_scale = jnp.exp(next_total + prev_peak - peak)
    next_scale = jnp.exp(next_peak - peak)
    return (
        prev_scale * prev_memory + next_scale * next_memory,
        prev_scale * prev_normer + next_scale * next_normer,
        prev_total + next_total,
        peak,
    )


def summary_kernel(info, key, value, ig, fg, out):
    heads = ig.shape[0]
    qk = key.shape[1] // heads
    hv = value.shape[1] // heads
    for h in range(heads):
        log_input, running = log_gates(ig[h : h + 1, :], fg[h : h + 1, :])
        total = running[:, -1:]
        lead = total - running + log_input
        peak = jnp.max(lead, axis=1, keepdims=True)
        weights = column(jnp.exp(lead - peak))
        weighted = key[:, h * qk : (h + 1) * qk].astype(f32) * weights
        memory = lax.dot_general(
            weighted.astype(bf16),
            value[:, h * hv : (h + 1) * hv],
            (((0,), (0,)), ((), ())),
            preferred_element_type=f32,
        )
        normer = jnp.sum(weighted, axis=0, keepdims=True)
        store_state(out, h, (memory, normer, total, peak))


def inner_kernel(info, query, key, value, ig, fg, numerator, side):
    heads = ig.shape[0]
    qk = key.shape[1] // heads
    hv = value.shape[1] // heads
    rows = key.shape[0]
    for h in range(heads):
        log_input, running = log_gates(ig[h : h + 1, :], fg[h : h + 1, :])
        running_column = column(running)
        causal = lax.broadcasted_iota(jnp.int32, (rows, rows), 0) >= lax.broadcasted_iota(
            jnp.int32, (rows, rows), 1
        )
        logs = jnp.where(causal, running_column - running + log_input, far_below)
        peak = jnp.max(logs, axis=1, keepdims=True)
        scores = lax.dot_general(
            query[:, h * qk : (h + 1) * qk] * bf16(qk**-0.5),
            key[:, h * qk : (h + 1) * qk],
            (((1,), (1,)), ((), ())),
            preferred_element_type=f32,
        ) * jnp.exp(logs - peak)
        numerator[:, h * hv : (h + 1) * hv] = jnp.dot(
            scores.astype(bf16), value[:, h * hv : (h + 1) * hv], preferred_element_type=f32
        )
        lane = lax.broadcasted_iota(jnp.int32, (rows, 128), 1)
        total = jnp.sum(scores, axis=1, keepdims=True)
        side[h] = jnp.where(lane == 0, total, jnp.where(lane == 1, peak, running_column))


def pair_kernel(info, mine, theirs, out):
    first = info[1] == 0
    for h in range(mine.shape[0]):
        own = load_state(mine, h)
        other = load_state(theirs, h)
        previous = tuple(jnp.where(first, a, b) for a, b in zip(own, other))
        following = tuple(jnp.where(first, b, a) for a, b in zip(own, other))
        store_state(out, h, combine(previous, following))


def combine_kernel(info, earlier, later, out):
    for h in range(earlier.shape[0]):
        store_state(out, h, combine(load_state(earlier, h), load_state(later, h)))


def output_kernel(has_pair, info, query, out_gate, numerator, side, *refs):
    states, keep, send = refs[:-2], refs[-2], refs[-1]
    heads = side.shape[0]
    qk = query.shape[1] // heads
    hv = out_gate.shape[1] // heads
    blocks = 2 * keep.shape[0]
    step = keep.shape[1]
    for h in range(heads):
        entering = None
        for i, ref in enumerate(states):
            state = load_state(ref, h)
            if has_pair and i == len(states) - 1:
                state = tuple(jnp.where(info[1] == 1, a, jnp.zeros_like(a)) for a in state)
            entering = state if entering is None else combine(entering, state)
        memory, normer, _, before = entering
        scaled = query[:, h * qk : (h + 1) * qk] * bf16(qk**-0.5)
        inner_total = side[h, :, 0:1]
        inner_peak = side[h, :, 1:2]
        carried = side[h, :, 2:3] + before
        peak = jnp.maximum(carried, inner_peak)
        outer = jnp.exp(carried - peak)
        inner = jnp.exp(inner_peak - peak)
        denominator = (
            outer * jnp.sum(scaled.astype(f32) * normer, axis=1, keepdims=True) + inner * inner_total
        )
        scale = 1.0 / jnp.maximum(jnp.abs(denominator), jnp.exp(-peak))
        top = outer * jnp.dot(scaled, memory.astype(bf16), preferred_element_type=f32)
        cell = (top + inner * numerator[:, h * hv : (h + 1) * hv]) * scale
        opened = cell * jax.nn.sigmoid(out_gate[:, h * hv : (h + 1) * hv].astype(f32))
        gated = opened.astype(bf16)
        for parity in range(2):

            @pl.when(info[3] == parity)
            def _():
                for j in range(blocks):
                    ref = keep if j % 2 == parity else send
                    ref[j // 2, :, h * hv : (h + 1) * hv] = gated[j * step : (j + 1) * step]


def project_kernel(shift, count, info, kept, got, own_weight, mate_weight, out):
    block = lax.rem(info[2] + shift, count)
    out[...] = (
        jnp.dot(kept[block], own_weight[...], preferred_element_type=f32)
        + jnp.dot(got[block], mate_weight[...], preferred_element_type=f32)
    ).astype(bf16)


def normalize(values, gains):
    return values * lax.rsqrt(jnp.mean(values * values, axis=-1, keepdims=True) + epsilon) * gains


def stream_kernel(info, residual, mix_gain, pre_gain, *refs):
    parts, stream_out, normed_out = refs[:-2], refs[-2], refs[-1]
    summed = parts[0][...].astype(f32)
    for part in parts[1:]:
        summed = summed + part[...].astype(f32)
    mixed = summed.astype(bf16).astype(f32)
    stream = (residual[...].astype(f32) + normalize(mixed, mix_gain[...])).astype(bf16)
    stream_out[...] = stream
    normed_out[...] = normalize(stream.astype(f32), pre_gain[...]).astype(bf16)


def result_kernel(info, stream, post_gain, *refs):
    parts, out = refs[:-1], refs[-1]
    summed = parts[0][...].astype(f32)
    for part in parts[1:]:
        summed = summed + part[...].astype(f32)
    ffn = summed.astype(bf16).astype(f32)
    out[...] = (stream[...].astype(f32) + normalize(ffn, post_gain[...])).astype(bf16)


def chunk_of(info, k, e, nz, pair):
    z = lax.rem(info[0] - k + nz, nz)
    return z * 2 + jnp.bitwise_xor(info[1], e) if pair else z


def up_kernel(order, nz, pair, ny, info, gate_taps, value_taps, *refs):
    halos = refs[: 2 * ny]
    pieces = refs[2 * ny : 4 * ny]
    blocks = refs[4 * ny : 4 * ny + len(order)]
    keep, send, rows_all, weight, up, sems = refs[4 * ny + len(order) :]
    rows = blocks[0].shape[1]
    copies = []
    for i, (k, e) in enumerate(order):
        start = pl.multiple_of(chunk_of(info, k, e, nz, pair) * rows, rows)
        copies.append(
            pltpu.make_async_copy(blocks[i], weight.at[:, pl.ds(start, rows), :], sems.at[i])
        )
        copies[-1].start()
    step = pieces[0].shape[0]
    total = step * 2 * ny
    halo = halos[0][...]
    for ref in halos[1:]:
        halo = halo + ref[...]
    rows_all[0:PAD, :] = halo
    for i in range(2 * ny):
        d, other = i // 2, i % 2
        chip = lax.rem(info[2] - d + ny, ny)
        core = 1 - info[3] if other else info[3]
        start = pl.multiple_of(PAD + (chip * 2 + core) * step, 16)
        rows_all[pl.ds(start, step), :] = pieces[i][...]
    for copy in copies:
        copy.wait()
    width = up.shape[2]
    tile = 256 if width % 256 == 0 else width
    for t in range(0, width, tile):
        for g in range(2):
            up[g, :, t : t + tile] = (
                jnp.dot(rows_all[...], weight[g, :, t : t + tile], preferred_element_type=f32)
                .astype(bf16)
                .astype(f32)
            )
        summed = []
        for g, taps in enumerate((gate_taps, value_taps)):
            first = PAD - CONV + 1
            conv = taps[0:1, t : t + tile] * up[g, first : first + total, t : t + tile]
            for j in range(1, CONV):
                conv = conv + taps[j : j + 1, t : t + tile] * (
                    up[g, first + j : first + j + total, t : t + tile]
                )
            summed.append(conv)
        hidden = (summed[0] / (1.0 + jnp.exp(-summed[0])) * summed[1]).astype(bf16)
        for parity in range(2):

            @pl.when(info[3] == parity)
            def _():
                for j in range(2 * ny):
                    ref = keep if j % 2 == parity else send
                    ref[j // 2, :, t : t + tile] = hidden[j * step : (j + 1) * step]


def down_kernel(order, nz, pair, info, hidden, *refs):
    blocks, out = refs[:-1], refs[-1]
    ny, step, width = hidden.shape
    flat = hidden[...].reshape(ny * step, width)
    rows = blocks[0].shape[0]
    for i, (k, e) in enumerate(order):
        start = pl.multiple_of(chunk_of(info, k, e, nz, pair) * rows, min(rows, 128))
        product = lax.dot_general(
            flat, blocks[i][...], (((1,), (1,)), ((), ())), preferred_element_type=f32
        ).astype(bf16)
        out[:, :, pl.ds(start, rows)] = product.reshape(ny, step, rows)


def add_kernel(info, mine, theirs, *outs):
    ny = mine.shape[0]
    for d in range(ny):
        block = lax.rem(info[2] + d, ny)
        outs[d][...] = (mine[block].astype(f32) + theirs[block].astype(f32)).astype(bf16)


def body(
    query_rows,
    key_rows,
    value_rows,
    out_gate_pre,
    input_gate_pre,
    forget_gate_pre,
    residual,
    out_proj,
    mix_gain,
    pre_gain,
    gate_proj,
    value_proj,
    gate_kernel,
    value_kernel,
    down_proj,
    post_gain,
):
    n_sp = lax.axis_size("sp")
    n_tp = lax.axis_size("tp")
    pair = n_sp % 2 == 0
    nz = n_sp // 2 if pair else n_sp
    ny = n_tp // 2
    rows, width = query_rows.shape[0], gate_proj.shape[1]
    heads = input_gate_pre.shape[0]
    qk = query_rows.shape[1] // heads
    hv = value_rows.shape[1] // heads
    model = residual.shape[1]
    step = rows // n_tp

    sp = lax.axis_index("sp")
    tp = lax.axis_index("tp")
    z, x = (sp // 2, sp % 2) if pair else (sp, 0 * sp)
    lane = lax.iota(jnp.int32, 8)
    info = jnp.where(
        lane == 0, z, jnp.where(lane == 1, x, jnp.where(lane == 2, tp // 2, tp % 2))
    ).astype(jnp.int32)

    stride = 2 if pair else 1
    ring = [(i, (i + stride) % n_sp) for i in range(n_sp)]
    along = lambda a: lax.ppermute(a, "sp", ring)
    across = lambda a: lax.ppermute(a, "sp", [(i, i ^ 1) for i in range(n_sp)])
    mate = lambda a: lax.ppermute(a, "tp", [(i, i ^ 1) for i in range(n_tp)])
    chips = lambda a, d: lax.ppermute(a, "tp", [(i, (i + 2 * d) % n_tp) for i in range(n_tp)])

    def spread(block):
        found = {(0, 0): block}
        if pair:
            found[0, 1] = across(block)
        for k in range(1, nz):
            found[k, 0] = along(found[k - 1, 0])
            if pair:
                found[k, 1] = across(found[k, 0])
        return found

    small = n_sp <= 16 and model // n_sp % 128 == 0
    up_own = jnp.stack((gate_proj, value_proj))
    if small:
        up_blocks = spread(up_own)
        down_blocks = spread(down_proj)
        wide, paired = nz, pair
    else:
        up_blocks = {(0, 0): lax.all_gather(up_own, "sp", axis=1, tiled=True)}
        down_blocks = {(0, 0): lax.all_gather(down_proj, "sp", axis=0, tiled=True)}
        wide, paired = 1, False
    order = tuple(up_blocks)
    mate_proj = mate(out_proj)

    summary = call(
        summary_kernel,
        ((heads, qk + 16, hv), bf16),
        "summary",
        (info, key_rows, value_rows, input_gate_pre, forget_gate_pre),
    )
    states = []
    total = summary
    if pair:
        partner = across(summary)
        total = call(pair_kernel, (summary.shape, bf16), "pair", (info, summary, partner))
        states.append(partner)
    reach = 1
    while reach < nz:
        route = [(i, i + stride * reach) for i in range(n_sp - stride * reach)]
        before = lax.ppermute(total, "sp", route)
        states.insert(0, before)
        reach *= 2
        if reach < nz:
            total = call(combine_kernel, (summary.shape, bf16), "combine", (info, before, total))
    inner, side = call(
        inner_kernel,
        (((rows, heads * hv), f32), ((heads, rows, 128), f32)),
        "inner",
        (info, query_rows, key_rows, value_rows, input_gate_pre, forget_gate_pre),
    )
    if not states:
        states = [jnp.zeros_like(summary)]
    kept, sent = call(
        functools.partial(output_kernel, pair),
        (((ny, step, heads * hv), bf16), ((ny, step, heads * hv), bf16)),
        "output",
        (info, query_rows, out_gate_pre, inner, side, *states),
    )
    got = mate(sent)

    parts = []
    for d in [*range(1, ny), 0]:
        part = call(
            functools.partial(project_kernel, d, ny),
            ((step, model), bf16),
            "project",
            (info, kept, got, out_proj, mate_proj),
        )
        parts.append(chips(part, d) if d else part)
    stream, normed = call(
        stream_kernel,
        (((step, model), bf16), ((step, model), bf16)),
        "stream",
        (info, residual, mix_gain[None], pre_gain[None], *parts),
    )

    pieces = []
    for d in range(ny):
        piece = chips(normed, d) if d else normed
        pieces += [piece, mate(piece)]
    halos = [
        lax.ppermute(
            normed[step - PAD :],
            ("sp", "tp"),
            [(i * n_tp + n_tp - 1, (i + 1) * n_tp + j) for i in range(n_sp - 1)],
        )
        for j in range(n_tp)
    ]

    up_spec = [SMEM, VMEM, VMEM] + [VMEM] * (2 * n_tp) + [HBM] * len(order)
    hidden_keep, hidden_send = call(
        functools.partial(up_kernel, order, wide, paired, ny),
        (((ny, step, width), bf16), ((ny, step, width), bf16)),
        "up",
        (info, gate_kernel, value_kernel, *halos, *pieces, *(up_blocks[o] for o in order)),
        scratch=(
            pltpu.VMEM((PAD + rows, model), bf16),
            pltpu.VMEM((2, model, width), bf16),
            pltpu.VMEM((2, PAD + rows, width), f32),
            pltpu.SemaphoreType.DMA((len(order),)),
        ),
        specs=up_spec,
    )
    down = functools.partial(down_kernel, order, wide, paired)
    down_args = tuple(down_blocks[o] for o in order)
    terms_send = call(down, ((ny, step, model), bf16), "down", (info, hidden_send, *down_args))
    terms_got = mate(terms_send)
    terms_keep = call(down, ((ny, step, model), bf16), "down", (info, hidden_keep, *down_args))
    sums = call(
        add_kernel,
        tuple(((step, model), bf16) for _ in range(ny)),
        "add",
        (info, terms_keep, terms_got),
    )
    parts = [chips(s, d) if d else s for d, s in enumerate(sums)]
    return call(
        result_kernel, ((step, model), bf16), "result", (info, stream, post_gain[None], *parts)
    )


def solution(mesh):
    return jax.shard_map(
        body,
        mesh=mesh,
        in_specs=(
            P("sp", "tp"),
            P("sp", "tp"),
            P("sp", "tp"),
            P("sp", "tp"),
            P("tp", "sp"),
            P("tp", "sp"),
            P(("sp", "tp"), None),
            P("tp", None),
            P(),
            P(),
            P("sp", "tp"),
            P("sp", "tp"),
            P(None, "tp"),
            P(None, "tp"),
            P("sp", "tp"),
            P(),
        ),
        out_specs=P(("sp", "tp"), None),
        check_vma=False,
    )
```

```python
import functools

import jax
import jax.numpy as jnp
from jax import lax
from jax.experimental import pallas as pl
from jax.experimental.pallas import tpu as pltpu
from jax.sharding import PartitionSpec as P

CONV = 3
PAD = 16
gate_cap = 15.0
epsilon = 1e-06
far_below = -1e30
f32 = jnp.float32
bf16 = jnp.bfloat16


SMEM = pl.BlockSpec(memory_space=pltpu.SMEM)
VMEM = pl.BlockSpec(memory_space=pltpu.VMEM)
HBM = pl.BlockSpec(memory_space=pltpu.HBM)


def call(kernel, out, args, scratch=(), mib=16, loads=False, outside=()):
    specs = [SMEM if i == 0 else HBM if i in outside else VMEM for i in range(len(args))]
    args = [
        a
        if i == 0 or loads
        else pltpu.with_memory_space_constraint(a, pltpu.HBM if i in outside else pltpu.VMEM)
        for i, a in enumerate(args)
    ]
    many = isinstance(out[0][0], tuple)
    return pl.pallas_call(
        kernel,
        out_shape=tuple(jax.ShapeDtypeStruct(*o) for o in out)
        if many
        else jax.ShapeDtypeStruct(*out),
        in_specs=specs,
        out_specs=tuple(VMEM for _ in out) if many else VMEM,
        scratch_shapes=list(scratch),
        compiler_params=pltpu.CompilerParams(vmem_limit_bytes=mib * 2**20),
    )(*args)


def softcap(values):
    return gate_cap * jnp.tanh(values / gate_cap)


def log_gates(ig, fg):
    log_input = softcap(ig)
    capped = softcap(fg)
    log_forget = jnp.minimum(capped, 0.0) - jnp.log1p(jnp.exp(-jnp.abs(capped)))
    rows = ig.shape[1]
    lane = lax.broadcasted_iota(jnp.int32, (8, rows), 1)
    running = jnp.broadcast_to(log_forget, (8, rows))
    reach = 1
    while reach < rows:
        running = running + jnp.where(lane >= reach, pltpu.roll(running, reach, 1), 0.0)
        reach *= 2
    running = running[:1]
    return log_input, running


def column(row):
    return jnp.broadcast_to(row, (128, row.shape[1])).T[:, :1]


def store_state(ref, h, state):
    memory, normer, total, peak = state
    rows, hv = memory.shape
    side = jnp.concatenate(
        (
            normer,
            jnp.broadcast_to(total, (1, 128)),
            jnp.broadcast_to(peak, (1, hv - rows - 128)),
        ),
        axis=1,
    )
    high = side.astype(bf16).astype(f32)
    middle = (side - high).astype(bf16).astype(f32)
    low = (side - high - middle).astype(bf16).astype(f32)
    tail = jnp.concatenate((high, middle, low, jnp.zeros((13, hv), f32)), axis=0)
    ref[h, :rows, :] = memory.astype(bf16)
    ref[h, rows:, :] = tail.astype(bf16)


def load_state(ref, h):
    rows = ref.shape[1] - 16
    tail = ref[h, rows:, :].astype(f32)
    side = tail[0:1] + tail[1:2] + tail[2:3]
    return (
        ref[h, :rows, :].astype(f32),
        side[:, :rows],
        side[:, rows : rows + 1],
        side[:, rows + 128 : rows + 129],
    )


def combine(previous, following):
    prev_memory, prev_normer, prev_total, prev_peak = previous
    next_memory, next_normer, next_total, next_peak = following
    peak = jnp.maximum(next_total + prev_peak, next_peak)
    prev_scale = jnp.exp(next_total + prev_peak - peak)
    next_scale = jnp.exp(next_peak - peak)
    return (
        prev_scale * prev_memory + next_scale * next_memory,
        prev_scale * prev_normer + next_scale * next_normer,
        prev_total + next_total,
        peak,
    )


def summary_kernel(info, key, value, ig, fg, stay, go):
    heads = ig.shape[0]
    qk = key.shape[1] // heads
    hv = value.shape[1] // heads
    for h in range(heads):
        log_input, running = log_gates(ig[h : h + 1, :], fg[h : h + 1, :])
        total = running[:, -1:]
        lead = total - running + log_input
        peak = jnp.max(lead, axis=1, keepdims=True)
        weights = column(jnp.exp(lead - peak))
        weighted = key[:, h * qk : (h + 1) * qk].astype(f32) * weights
        memory = lax.dot_general(
            weighted.astype(bf16),
            value[:, h * hv : (h + 1) * hv],
            (((0,), (0,)), ((), ())),
            preferred_element_type=f32,
        )
        normer = jnp.sum(weighted, axis=0, keepdims=True)
        half = qk // 2
        halves = [
            (memory[:half], normer[:, :half], total, peak),
            (memory[half:], normer[:, half:], total, peak),
        ]
        for parity in range(2):

            @pl.when(info[1] == parity)
            def _():
                store_state(stay, h, halves[parity])
                store_state(go, h, halves[1 - parity])


def inner_kernel(info, query, key, value, ig, fg, numerator, side):
    heads = ig.shape[0]
    qk = key.shape[1] // heads
    hv = value.shape[1] // heads
    rows = key.shape[0]
    for h in range(heads):
        log_input, running = log_gates(ig[h : h + 1, :], fg[h : h + 1, :])
        running_column = column(running)
        causal = lax.broadcasted_iota(jnp.int32, (rows, rows), 0) >= lax.broadcasted_iota(
            jnp.int32, (rows, rows), 1
        )
        logs = jnp.where(causal, running_column - running + log_input, far_below)
        peak = jnp.max(logs, axis=1, keepdims=True)
        scores = lax.dot_general(
            query[:, h * qk : (h + 1) * qk] * bf16(qk**-0.5),
            key[:, h * qk : (h + 1) * qk],
            (((1,), (1,)), ((), ())),
            preferred_element_type=f32,
        ) * jnp.exp(logs - peak)
        numerator[:, h * hv : (h + 1) * hv] = jnp.dot(
            scores.astype(bf16), value[:, h * hv : (h + 1) * hv], preferred_element_type=f32
        )
        lane = lax.broadcasted_iota(jnp.int32, (rows, 128), 1)
        total = jnp.sum(scores, axis=1, keepdims=True)
        side[h] = jnp.where(lane == 0, total, jnp.where(lane == 1, peak, running_column))


def pair_kernel(info, mine, theirs, out):
    first = info[1] == 0
    for h in range(mine.shape[0]):
        own = load_state(mine, h)
        other = load_state(theirs, h)
        previous = tuple(jnp.where(first, a, b) for a, b in zip(own, other))
        following = tuple(jnp.where(first, b, a) for a, b in zip(own, other))
        store_state(out, h, combine(previous, following))


def combine_kernel(info, earlier, later, out):
    for h in range(earlier.shape[0]):
        store_state(out, h, combine(load_state(earlier, h), load_state(later, h)))


def entering_kernel(info, mine, theirs, *refs):
    states, keep, send = refs[:-2], refs[-2], refs[-1]
    first = info[1] == 0
    for h in range(mine.shape[0]):
        opening = tuple(
            jnp.where(first, a, b) for a, b in zip(load_state(mine, h), load_state(theirs, h))
        )
        before = None
        for ref in states:
            state = load_state(ref, h)
            before = state if before is None else combine(before, state)
        if before is None:
            before = tuple(jnp.zeros_like(a) for a in opening)
        after = combine(before, opening)
        store_state(keep, h, tuple(jnp.where(first, a, b) for a, b in zip(before, after)))
        store_state(send, h, tuple(jnp.where(first, b, a) for a, b in zip(before, after)))


def output_kernel(info, query, out_gate, numerator, side, mine, theirs, keep, send):
    heads = side.shape[0]
    qk = query.shape[1] // heads
    hv = out_gate.shape[1] // heads
    half = qk // 2
    blocks = 2 * keep.shape[0]
    step = keep.shape[1]
    for h in range(heads):
        own_half = pl.multiple_of(h * qk + info[1] * half, half)
        other_half = pl.multiple_of(h * qk + (1 - info[1]) * half, half)
        own_query = query[:, pl.ds(own_half, half)] * bf16(qk**-0.5)
        other_query = query[:, pl.ds(other_half, half)] * bf16(qk**-0.5)
        _, own_normer, _, before = load_state(mine, h)
        _, other_normer, _, _ = load_state(theirs, h)
        top = jnp.dot(own_query, mine[h, :half, :], preferred_element_type=f32) + jnp.dot(
            other_query, theirs[h, :half, :], preferred_element_type=f32
        )
        bottom = jnp.sum(
            own_query.astype(f32) * own_normer + other_query.astype(f32) * other_normer,
            axis=1,
            keepdims=True,
        )
        inner_total = side[h, :, 0:1]
        inner_peak = side[h, :, 1:2]
        carried = side[h, :, 2:3] + before
        peak = jnp.maximum(carried, inner_peak)
        outer = jnp.exp(carried - peak)
        inner = jnp.exp(inner_peak - peak)
        denominator = outer * bottom + inner * inner_total
        scale = 1.0 / jnp.maximum(jnp.abs(denominator), jnp.exp(-peak))
        cell = (outer * top + inner * numerator[:, h * hv : (h + 1) * hv]) * scale
        opened = cell * jax.nn.sigmoid(out_gate[:, h * hv : (h + 1) * hv].astype(f32))
        gated = opened.astype(bf16)
        for parity in range(2):

            @pl.when(info[3] == parity)
            def _():
                for j in range(blocks):
                    ref = keep if j % 2 == parity else send
                    ref[j // 2, :, h * hv : (h + 1) * hv] = gated[j * step : (j + 1) * step]


def project_kernel(shift, count, info, kept, got, own_weight, mate_weight, out):
    block = lax.rem(info[2] + shift, count)
    out[...] = (
        jnp.dot(kept[block], own_weight[...], preferred_element_type=f32)
        + jnp.dot(got[block], mate_weight[...], preferred_element_type=f32)
    ).astype(bf16)


def normalize(values, gains):
    return values * lax.rsqrt(jnp.mean(values * values, axis=-1, keepdims=True) + epsilon) * gains


def stream_kernel(info, residual, mix_gain, pre_gain, *refs):
    parts, stream_out, normed_out = refs[:-2], refs[-2], refs[-1]
    summed = parts[0][...].astype(f32)
    for part in parts[1:]:
        summed = summed + part[...].astype(f32)
    mixed = summed.astype(bf16).astype(f32)
    stream = (residual[...].astype(f32) + normalize(mixed, mix_gain[...])).astype(bf16)
    stream_out[...] = stream
    normed_out[...] = normalize(stream.astype(f32), pre_gain[...]).astype(bf16)


def chunk_of(info, k, e, nz, pair):
    z = lax.rem(info[0] - k + nz, nz)
    return z * 2 + jnp.bitwise_xor(info[1], e) if pair else z


def tiles_of(width):
    tile = 256 if width % 256 == 0 else width
    return [slice(t, t + tile) for t in range(0, width, tile)]


def times_weight(order, nz, pair, info, rows_all, blocks, span):
    rows = blocks[0].shape[0]
    product = None
    for (k, e), block in zip(order, blocks):
        start = pl.multiple_of(chunk_of(info, k, e, nz, pair) * rows, min(rows, 128))
        term = jnp.dot(
            rows_all[:, pl.ds(start, rows)], block[:, span], preferred_element_type=f32
        )
        product = term if product is None else product + term
    return product.astype(bf16)


def gate_kernel_(order, nz, pair, ny, info, *refs):
    halos = refs[:ny]
    pieces = refs[ny : 3 * ny]
    blocks = refs[3 * ny : 3 * ny + len(order)]
    out, rows_all, own, sem = refs[3 * ny + len(order) :]
    copy = pltpu.make_async_copy(blocks[0], own, sem)
    copy.start()
    blocks = (*blocks[1:], own)
    order = (*order[1:], order[0])
    halo = halos[0][...]
    for ref in halos[1:]:
        halo = halo + ref[...]
    rows_all[0:PAD, :] = halo
    step = pieces[0].shape[0]
    for i, piece in enumerate(pieces):
        d, other = i // 2, i % 2
        chip = lax.rem(info[2] - d + ny, ny)
        core = 1 - info[3] if other else info[3]
        start = pl.multiple_of(PAD + (chip * 2 + core) * step, 16)
        rows_all[pl.ds(start, step), :] = piece[...]
    copy.wait()
    for span in tiles_of(out.shape[1]):
        out[:, span] = times_weight(order, nz, pair, info, rows_all, blocks, span)


def up_kernel(order, nz, pair, info, gate_taps, value_taps, rows_all, gates, *refs):
    blocks = refs[: len(order)]
    keep, send, up = refs[len(order) :]
    ny, step, width = keep.shape
    total = 2 * ny * step
    up[0] = gates[...].astype(f32)
    for span in tiles_of(width):
        up[1, :, span] = times_weight(order, nz, pair, info, rows_all, blocks, span).astype(f32)
        summed = []
        for g, taps in enumerate((gate_taps, value_taps)):
            first = PAD - CONV + 1
            conv = taps[0:1, span] * up[g, first : first + total, span]
            for j in range(1, CONV):
                conv = conv + taps[j : j + 1, span] * up[g, first + j : first + j + total, span]
            summed.append(conv)
        hidden = (summed[0] / (1.0 + jnp.exp(-summed[0])) * summed[1]).astype(bf16)
        for parity in range(2):

            @pl.when(info[3] == parity)
            def _():
                for j in range(2 * ny):
                    ref = keep if j % 2 == parity else send
                    ref[j // 2, :, span] = hidden[j * step : (j + 1) * step]


def down_kernel(shift, info, keep, send, *refs):
    blocks, keep_out, send_out = refs[:-2], refs[-2], refs[-1]
    chip = lax.rem(info[2] + shift, keep.shape[0])
    step = keep.shape[1]
    both = jnp.concatenate((keep[chip], send[chip]), axis=0)
    start = 0
    for block in blocks:
        end = start + block.shape[0]
        product = lax.dot_general(
            both, block[...], (((1,), (1,)), ((), ())), preferred_element_type=f32
        ).astype(bf16)
        keep_out[:, start:end] = product[:step]
        send_out[:, start:end] = product[step:]
        start = end


def result_kernel(groups, rows, nz, pair, info, stream, post_gain, *refs):
    out, summed = refs[-2], refs[-1]
    count = (len(refs) - 2) // len(groups)
    for g, order in enumerate(groups):
        parts = refs[g * count : (g + 1) * count]
        total = parts[0][...].astype(f32)
        for part in parts[1:]:
            total = total + part[...].astype(f32)
        for i, (k, e) in enumerate(order):
            start = pl.multiple_of(chunk_of(info, k, e, nz, pair) * rows, min(rows, 128))
            summed[:, pl.ds(start, rows)] = total[:, i * rows : (i + 1) * rows]
    ffn = summed[...].astype(bf16).astype(f32)
    out[...] = (stream[...].astype(f32) + normalize(ffn, post_gain[...])).astype(bf16)


def is_small(n_sp, model):
    return n_sp <= 16 and model // n_sp % 128 == 0


def layer(
    query_rows,
    key_rows,
    value_rows,
    out_gate_pre,
    input_gate_pre,
    forget_gate_pre,
    residual,
    out_proj,
    mix_gain,
    pre_gain,
    gate_proj,
    value_proj,
    gate_kernel,
    value_kernel,
    down_proj,
    post_gain,
):
    n_sp = lax.axis_size("sp")
    n_tp = lax.axis_size("tp")
    nz = n_sp // 2
    ny = n_tp // 2
    rows, width = query_rows.shape[0], gate_proj.shape[1]
    heads = input_gate_pre.shape[0]
    qk = query_rows.shape[1] // heads
    hv = value_rows.shape[1] // heads
    model = residual.shape[1]
    step = rows // n_tp

    sp = lax.axis_index("sp")
    tp = lax.axis_index("tp")
    z, x = sp // 2, sp % 2
    lane = lax.iota(jnp.int32, 8)
    info = jnp.where(
        lane == 0, z, jnp.where(lane == 1, x, jnp.where(lane == 2, tp // 2, tp % 2))
    ).astype(jnp.int32)

    ring = [(i, (i + 2) % n_sp) for i in range(n_sp)]
    swap = [(i, i ^ 1) for i in range(n_sp)]

    mate = lambda a: lax.ppermute(a, "tp", [(i, i ^ 1) for i in range(n_tp)])
    chips = lambda a, d: lax.ppermute(a, "tp", [(i, (i + 2 * d) % n_tp) for i in range(n_tp)])

    def spread(block, name):
        found = {(0, 0): block}
        for k in range(nz):
            if k:
                found[k, 0] = lax.ppermute(found[k - 1, 0], "sp", ring)
            if name == "d" and k == 1:
                found[k, 1] = lax.ppermute(found[0, 1], "sp", ring)
            else:
                found[k, 1] = lax.ppermute(found[k, 0], "sp", swap)
        return found

    small = is_small(n_sp, model)
    if small:
        gates, values, downs = (
            spread(w, name)
            for w, name in ((gate_proj, "g"), (value_proj, "v"), (down_proj, "d"))
        )
        wide, paired = nz, True
    else:
        gates, values, downs = (
            {(0, 0): lax.all_gather(w, "sp", axis=0, tiled=True)}
            for w in (gate_proj, value_proj, down_proj)
        )
        wide, paired = 1, False
    order = tuple(gates)
    mate_proj = mate(out_proj)

    half_state = ((heads, qk // 2 + 16, hv), bf16)
    stay, go = call(
        summary_kernel,
        (half_state, half_state),
        (info, key_rows, value_rows, input_gate_pre, forget_gate_pre),
        loads=True,
    )
    partner = lax.ppermute(go, "sp", swap)
    total = call(pair_kernel, half_state, (info, stay, partner))
    states = []
    reach = 1
    while reach < nz:
        route = [(i, i + 2 * reach) for i in range(n_sp - 2 * reach)]
        states.insert(0, lax.ppermute(total, "sp", route))
        reach *= 2
        if reach < nz:
            total = call(combine_kernel, half_state, (info, states[0], total))
    before, across = call(entering_kernel, (half_state, half_state), (info, stay, partner, *states))
    across = lax.ppermute(across, "sp", swap)
    inner, side = call(
        inner_kernel,
        (((rows, heads * hv), f32), ((heads, rows, 128), f32)),
        (info, query_rows, key_rows, value_rows, input_gate_pre, forget_gate_pre),
    )
    kept, sent = call(
        output_kernel,
        (((ny, step, heads * hv), bf16), ((ny, step, heads * hv), bf16)),
        (info, query_rows, out_gate_pre, inner, side, before, across),
    )
    got = mate(sent)

    parts = []
    for d in [*range(1, ny), 0]:
        part = call(
            functools.partial(project_kernel, d, ny),
            ((step, model), bf16),
            (info, kept, got, out_proj, mate_proj),
        )
        parts.append(chips(part, d) if d else part)
    stream, normed = call(
        stream_kernel,
        (((step, model), bf16), ((step, model), bf16)),
        (info, residual, mix_gain[None], pre_gain[None], *parts),
    )

    pieces = []
    for d in range(ny):
        piece = chips(normed, d) if d else normed
        pieces += [piece, mate(piece)]
    last_rows = jnp.where(tp % 2 == 1, normed[step - PAD :], pieces[1][step - PAD :])
    halos = [
        lax.ppermute(
            last_rows,
            ("sp", "tp"),
            [
                (i * n_tp + n_tp - 2 + c, (i + 1) * n_tp + 2 * j + c)
                for i in range(n_sp - 1)
                for c in range(2)
            ],
        )
        for j in range(ny)
    ]

    up_gate, group_rows = call(
        functools.partial(gate_kernel_, order, wide, paired, ny),
        (((PAD + rows, width), bf16), ((PAD + rows, model), bf16)),
        (info, *halos, *pieces, *(gates[o] for o in order)),
        scratch=(pltpu.VMEM((model // len(order), width), bf16), pltpu.SemaphoreType.DMA),
        outside=(1 + ny + n_tp,),
    )
    hidden_keep, hidden_send = call(
        functools.partial(up_kernel, order, wide, paired),
        (((ny, step, width), bf16), ((ny, step, width), bf16)),
        (info, gate_kernel, value_kernel, group_rows, up_gate, *(values[o] for o in order)),
        scratch=(pltpu.VMEM((2, PAD + rows, width), f32),),
    )
    arrival = sorted(order, key=lambda o: o[0] + o[1] * {0: 1, 1: nz + 1}.get(o[0], nz - 1))
    cuts = [len(arrival) * i // 4 for i in (0, 2, 3, 4)]
    groups = [arrival[a:b] for a, b in zip(cuts, cuts[1:]) if b > a]
    rows_of = model // len(order)
    parts = [[] for _ in groups]
    for d in [*range(1, ny), 0]:
        for g, blocks in enumerate(groups):
            shape = ((step, rows_of * len(blocks)), bf16)
            mine, away = call(
                functools.partial(down_kernel, d),
                (shape, shape),
                (info, hidden_keep, hidden_send, *(downs[o] for o in blocks)),
            )
            theirs = mate(away)
            if d:
                both = (mine.astype(f32) + theirs.astype(f32)).astype(bf16)
                route = [(i, (i + 2 * d) % n_tp) for i in range(n_tp)]
                parts[g].append(lax.ppermute(both, "tp", route))
            else:
                parts[g] += [mine, theirs]
    return call(
        functools.partial(result_kernel, groups, rows_of, wide, paired),
        ((step, model), bf16),
        (info, stream, post_gain[None], *(p for group in parts for p in group)),
        scratch=(pltpu.VMEM((step, model), f32),),
    )


def solution(mesh):
    return jax.shard_map(
        layer,
        mesh=mesh,
        in_specs=(
            P("sp", "tp"),
            P("sp", "tp"),
            P("sp", "tp"),
            P("sp", "tp"),
            P("tp", "sp"),
            P("tp", "sp"),
            P(("sp", "tp"), None),
            P("tp", None),
            P(),
            P(),
            P("sp", "tp"),
            P("sp", "tp"),
            P(None, "tp"),
            P(None, "tp"),
            P("sp", "tp"),
            P(),
        ),
        out_specs=P(("sp", "tp"), None),
        check_vma=False,
    )
```

```python
import functools

import jax
import jax.numpy as jnp
from jax import lax
from jax.experimental import pallas as pl
from jax.experimental.pallas import tpu as pltpu
from jax.sharding import PartitionSpec as P

CONV = 3
PAD = 16
gate_cap = 15.0
epsilon = 1e-06
far_below = -1e30
f32 = jnp.float32
bf16 = jnp.bfloat16


SMEM = pl.BlockSpec(memory_space=pltpu.SMEM)
VMEM = pl.BlockSpec(memory_space=pltpu.VMEM)
HBM = pl.BlockSpec(memory_space=pltpu.HBM)


def call(kernel, out, args, scratch=(), mib=16, loads=False, outside=()):
    specs = [SMEM if i == 0 else HBM if i in outside else VMEM for i in range(len(args))]
    args = [
        a
        if i == 0 or loads
        else pltpu.with_memory_space_constraint(a, pltpu.HBM if i in outside else pltpu.VMEM)
        for i, a in enumerate(args)
    ]
    many = isinstance(out[0][0], tuple)
    return pl.pallas_call(
        kernel,
        out_shape=tuple(jax.ShapeDtypeStruct(*o) for o in out)
        if many
        else jax.ShapeDtypeStruct(*out),
        in_specs=specs,
        out_specs=tuple(VMEM for _ in out) if many else VMEM,
        scratch_shapes=list(scratch),
        compiler_params=pltpu.CompilerParams(vmem_limit_bytes=mib * 2**20),
    )(*args)


def softcap(values):
    return gate_cap * jnp.tanh(values / gate_cap)


def log_gates(ig, fg):
    log_input = softcap(ig)
    capped = softcap(fg)
    log_forget = jnp.minimum(capped, 0.0) - jnp.log1p(jnp.exp(-jnp.abs(capped)))
    rows = ig.shape[1]
    lane = lax.broadcasted_iota(jnp.int32, (8, rows), 1)
    running = jnp.broadcast_to(log_forget, (8, rows))
    reach = 1
    while reach < rows:
        running = running + jnp.where(lane >= reach, pltpu.roll(running, reach, 1), 0.0)
        reach *= 2
    running = running[:1]
    return log_input, running


def column(row):
    return jnp.broadcast_to(row, (128, row.shape[1])).T[:, :1]


def store_state(ref, h, state):
    memory, normer, total, peak = state
    rows, hv = memory.shape
    side = jnp.concatenate(
        (
            normer,
            jnp.broadcast_to(total, (1, 128)),
            jnp.broadcast_to(peak, (1, hv - rows - 128)),
        ),
        axis=1,
    )
    high = side.astype(bf16).astype(f32)
    middle = (side - high).astype(bf16).astype(f32)
    low = (side - high - middle).astype(bf16).astype(f32)
    tail = jnp.concatenate((high, middle, low, jnp.zeros((13, hv), f32)), axis=0)
    ref[h, :rows, :] = memory.astype(bf16)
    ref[h, rows:, :] = tail.astype(bf16)


def load_state(ref, h):
    rows = ref.shape[1] - 16
    tail = ref[h, rows:, :].astype(f32)
    side = tail[0:1] + tail[1:2] + tail[2:3]
    return (
        ref[h, :rows, :].astype(f32),
        side[:, :rows],
        side[:, rows : rows + 1],
        side[:, rows + 128 : rows + 129],
    )


def combine(previous, following):
    prev_memory, prev_normer, prev_total, prev_peak = previous
    next_memory, next_normer, next_total, next_peak = following
    peak = jnp.maximum(next_total + prev_peak, next_peak)
    prev_scale = jnp.exp(next_total + prev_peak - peak)
    next_scale = jnp.exp(next_peak - peak)
    return (
        prev_scale * prev_memory + next_scale * next_memory,
        prev_scale * prev_normer + next_scale * next_normer,
        prev_total + next_total,
        peak,
    )


def summary_kernel(info, key, value, ig, fg, stay, go):
    heads = ig.shape[0]
    qk = key.shape[1] // heads
    hv = value.shape[1] // heads
    for h in range(heads):
        log_input, running = log_gates(ig[h : h + 1, :], fg[h : h + 1, :])
        total = running[:, -1:]
        lead = total - running + log_input
        peak = jnp.max(lead, axis=1, keepdims=True)
        weights = column(jnp.exp(lead - peak))
        weighted = key[:, h * qk : (h + 1) * qk].astype(f32) * weights
        memory = lax.dot_general(
            weighted.astype(bf16),
            value[:, h * hv : (h + 1) * hv],
            (((0,), (0,)), ((), ())),
            preferred_element_type=f32,
        )
        normer = jnp.sum(weighted, axis=0, keepdims=True)
        half = qk // 2
        halves = [
            (memory[:half], normer[:, :half], total, peak),
            (memory[half:], normer[:, half:], total, peak),
        ]
        for parity in range(2):

            @pl.when(info[1] == parity)
            def _():
                store_state(stay, h, halves[parity])
                store_state(go, h, halves[1 - parity])


def inner_kernel(info, query, key, value, ig, fg, numerator, side):
    heads = ig.shape[0]
    qk = key.shape[1] // heads
    hv = value.shape[1] // heads
    rows = key.shape[0]
    for h in range(heads):
        log_input, running = log_gates(ig[h : h + 1, :], fg[h : h + 1, :])
        running_column = column(running)
        causal = lax.broadcasted_iota(jnp.int32, (rows, rows), 0) >= lax.broadcasted_iota(
            jnp.int32, (rows, rows), 1
        )
        logs = jnp.where(causal, running_column - running + log_input, far_below)
        peak = jnp.max(logs, axis=1, keepdims=True)
        scores = lax.dot_general(
            query[:, h * qk : (h + 1) * qk] * bf16(qk**-0.5),
            key[:, h * qk : (h + 1) * qk],
            (((1,), (1,)), ((), ())),
            preferred_element_type=f32,
        ) * jnp.exp(logs - peak)
        numerator[:, h * hv : (h + 1) * hv] = jnp.dot(
            scores.astype(bf16), value[:, h * hv : (h + 1) * hv], preferred_element_type=f32
        )
        lane = lax.broadcasted_iota(jnp.int32, (rows, 128), 1)
        total = jnp.sum(scores, axis=1, keepdims=True)
        side[h] = jnp.where(lane == 0, total, jnp.where(lane == 1, peak, running_column))


def pair_kernel(info, mine, theirs, out):
    first = info[1] == 0
    for h in range(mine.shape[0]):
        own = load_state(mine, h)
        other = load_state(theirs, h)
        previous = tuple(jnp.where(first, a, b) for a, b in zip(own, other))
        following = tuple(jnp.where(first, b, a) for a, b in zip(own, other))
        store_state(out, h, combine(previous, following))


def combine_kernel(info, earlier, later, out):
    for h in range(earlier.shape[0]):
        store_state(out, h, combine(load_state(earlier, h), load_state(later, h)))


def entering_kernel(info, mine, theirs, *refs):
    states, keep, send = refs[:-2], refs[-2], refs[-1]
    first = info[1] == 0
    for h in range(mine.shape[0]):
        opening = tuple(
            jnp.where(first, a, b) for a, b in zip(load_state(mine, h), load_state(theirs, h))
        )
        before = None
        for ref in states:
            state = load_state(ref, h)
            before = state if before is None else combine(before, state)
        if before is None:
            before = tuple(jnp.zeros_like(a) for a in opening)
        after = combine(before, opening)
        store_state(keep, h, tuple(jnp.where(first, a, b) for a, b in zip(before, after)))
        store_state(send, h, tuple(jnp.where(first, b, a) for a, b in zip(before, after)))


def output_kernel(info, query, out_gate, numerator, side, mine, theirs, keep, send):
    heads = side.shape[0]
    qk = query.shape[1] // heads
    hv = out_gate.shape[1] // heads
    half = qk // 2
    blocks = 2 * keep.shape[0]
    step = keep.shape[1]
    for h in range(heads):
        own_half = pl.multiple_of(h * qk + info[1] * half, half)
        other_half = pl.multiple_of(h * qk + (1 - info[1]) * half, half)
        own_query = query[:, pl.ds(own_half, half)] * bf16(qk**-0.5)
        other_query = query[:, pl.ds(other_half, half)] * bf16(qk**-0.5)
        _, own_normer, _, before = load_state(mine, h)
        _, other_normer, _, _ = load_state(theirs, h)
        top = jnp.dot(own_query, mine[h, :half, :], preferred_element_type=f32) + jnp.dot(
            other_query, theirs[h, :half, :], preferred_element_type=f32
        )
        bottom = jnp.sum(
            own_query.astype(f32) * own_normer + other_query.astype(f32) * other_normer,
            axis=1,
            keepdims=True,
        )
        inner_total = side[h, :, 0:1]
        inner_peak = side[h, :, 1:2]
        carried = side[h, :, 2:3] + before
        peak = jnp.maximum(carried, inner_peak)
        outer = jnp.exp(carried - peak)
        inner = jnp.exp(inner_peak - peak)
        denominator = outer * bottom + inner * inner_total
        scale = 1.0 / jnp.maximum(jnp.abs(denominator), jnp.exp(-peak))
        cell = (outer * top + inner * numerator[:, h * hv : (h + 1) * hv]) * scale
        opened = cell * jax.nn.sigmoid(out_gate[:, h * hv : (h + 1) * hv].astype(f32))
        gated = opened.astype(bf16)
        for parity in range(2):

            @pl.when(info[3] == parity)
            def _():
                for j in range(blocks):
                    ref = keep if j % 2 == parity else send
                    ref[j // 2, :, h * hv : (h + 1) * hv] = gated[j * step : (j + 1) * step]


def project_kernel(shift, count, info, kept, got, own_weight, mate_weight, out):
    block = lax.rem(info[2] + shift, count)
    out[...] = (
        jnp.dot(kept[block], own_weight[...], preferred_element_type=f32)
        + jnp.dot(got[block], mate_weight[...], preferred_element_type=f32)
    ).astype(bf16)


def normalize(values, gains):
    return values * lax.rsqrt(jnp.mean(values * values, axis=-1, keepdims=True) + epsilon) * gains


def stream_kernel(info, residual, mix_gain, pre_gain, *refs):
    parts, stream_out, normed_out = refs[:-2], refs[-2], refs[-1]
    summed = parts[0][...].astype(f32)
    for part in parts[1:]:
        summed = summed + part[...].astype(f32)
    mixed = summed.astype(bf16).astype(f32)
    stream = (residual[...].astype(f32) + normalize(mixed, mix_gain[...])).astype(bf16)
    stream_out[...] = stream
    normed_out[...] = normalize(stream.astype(f32), pre_gain[...]).astype(bf16)


def chunk_of(info, k, e, nz, pair):
    z = lax.rem(info[0] - k + nz, nz)
    return z * 2 + jnp.bitwise_xor(info[1], e) if pair else z


def tiles_of(width):
    tile = 256 if width % 256 == 0 else width
    return [slice(t, t + tile) for t in range(0, width, tile)]


def times_weight(order, nz, pair, info, rows_all, blocks, span):
    rows = blocks[0].shape[0]
    product = None
    for (k, e), block in zip(order, blocks):
        start = pl.multiple_of(chunk_of(info, k, e, nz, pair) * rows, min(rows, 128))
        term = jnp.dot(
            rows_all[:, pl.ds(start, rows)], block[:, span], preferred_element_type=f32
        )
        product = term if product is None else product + term
    return product.astype(bf16)


def gate_kernel_(order, nz, pair, ny, info, *refs):
    halos = refs[:ny]
    pieces = refs[ny : 3 * ny]
    blocks = refs[3 * ny : 3 * ny + len(order)]
    out, rows_all, own, sem = refs[3 * ny + len(order) :]
    copy = pltpu.make_async_copy(blocks[0], own, sem)
    copy.start()
    blocks = (*blocks[1:], own)
    order = (*order[1:], order[0])
    halo = halos[0][...]
    for ref in halos[1:]:
        halo = halo + ref[...]
    rows_all[0:PAD, :] = halo
    step = pieces[0].shape[0]
    for i, piece in enumerate(pieces):
        d, other = i // 2, i % 2
        chip = lax.rem(info[2] - d + ny, ny)
        core = 1 - info[3] if other else info[3]
        start = pl.multiple_of(PAD + (chip * 2 + core) * step, 16)
        rows_all[pl.ds(start, step), :] = piece[...]
    copy.wait()
    for span in tiles_of(out.shape[1]):
        out[:, span] = times_weight(order, nz, pair, info, rows_all, blocks, span)


def up_kernel(order, nz, pair, info, gate_taps, value_taps, rows_all, gates, *refs):
    blocks = refs[: len(order)]
    keep, send, up = refs[len(order) :]
    ny, step, width = keep.shape
    total = 2 * ny * step
    up[0] = gates[...].astype(f32)
    for span in tiles_of(width):
        up[1, :, span] = times_weight(order, nz, pair, info, rows_all, blocks, span).astype(f32)
        summed = []
        for g, taps in enumerate((gate_taps, value_taps)):
            first = PAD - CONV + 1
            conv = taps[0:1, span] * up[g, first : first + total, span]
            for j in range(1, CONV):
                conv = conv + taps[j : j + 1, span] * up[g, first + j : first + j + total, span]
            summed.append(conv)
        hidden = (summed[0] / (1.0 + jnp.exp(-summed[0])) * summed[1]).astype(bf16)
        for parity in range(2):

            @pl.when(info[3] == parity)
            def _():
                for j in range(2 * ny):
                    ref = keep if j % 2 == parity else send
                    ref[j // 2, :, span] = hidden[j * step : (j + 1) * step]


def down_kernel(shift, info, keep, send, *refs):
    blocks, keep_out, send_out = refs[:-2], refs[-2], refs[-1]
    chip = lax.rem(info[2] + shift, keep.shape[0])
    step = keep.shape[1]
    both = jnp.concatenate((keep[chip], send[chip]), axis=0)
    start = 0
    for block in blocks:
        end = start + block.shape[0]
        product = lax.dot_general(
            both, block[...], (((1,), (1,)), ((), ())), preferred_element_type=f32
        ).astype(bf16)
        keep_out[:, start:end] = product[:step]
        send_out[:, start:end] = product[step:]
        start = end


def add_kernel(info, mine, theirs, out):
    out[...] = (mine[...].astype(f32) + theirs[...].astype(f32)).astype(bf16)


def result_kernel(groups, rows, nz, pair, info, stream, post_gain, *refs):
    out, summed = refs[-2], refs[-1]
    count = (len(refs) - 2) // len(groups)
    for g, order in enumerate(groups):
        parts = refs[g * count : (g + 1) * count]
        total = parts[0][...].astype(f32)
        for part in parts[1:]:
            total = total + part[...].astype(f32)
        for i, (k, e) in enumerate(order):
            start = pl.multiple_of(chunk_of(info, k, e, nz, pair) * rows, min(rows, 128))
            summed[:, pl.ds(start, rows)] = total[:, i * rows : (i + 1) * rows]
    ffn = summed[...].astype(bf16).astype(f32)
    out[...] = (stream[...].astype(f32) + normalize(ffn, post_gain[...])).astype(bf16)


def is_small(n_sp, model):
    return n_sp <= 16 and model // n_sp % 128 == 0


def layer(
    query_rows,
    key_rows,
    value_rows,
    out_gate_pre,
    input_gate_pre,
    forget_gate_pre,
    residual,
    out_proj,
    mix_gain,
    pre_gain,
    gate_proj,
    value_proj,
    gate_kernel,
    value_kernel,
    down_proj,
    post_gain,
):
    n_sp = lax.axis_size("sp")
    n_tp = lax.axis_size("tp")
    nz = n_sp // 2
    ny = n_tp // 2
    rows, width = query_rows.shape[0], gate_proj.shape[1]
    heads = input_gate_pre.shape[0]
    qk = query_rows.shape[1] // heads
    hv = value_rows.shape[1] // heads
    model = residual.shape[1]
    step = rows // n_tp

    sp = lax.axis_index("sp")
    tp = lax.axis_index("tp")
    z, x = sp // 2, sp % 2
    lane = lax.iota(jnp.int32, 8)
    info = jnp.where(
        lane == 0, z, jnp.where(lane == 1, x, jnp.where(lane == 2, tp // 2, tp % 2))
    ).astype(jnp.int32)

    ring = [(i, (i + 2) % n_sp) for i in range(n_sp)]
    swap = [(i, i ^ 1) for i in range(n_sp)]

    mate = lambda a: lax.ppermute(a, "tp", [(i, i ^ 1) for i in range(n_tp)])
    chips = lambda a, d: lax.ppermute(a, "tp", [(i, (i + 2 * d) % n_tp) for i in range(n_tp)])

    def spread(block, name):
        found = {(0, 0): block}
        for k in range(nz):
            if k:
                found[k, 0] = lax.ppermute(found[k - 1, 0], "sp", ring)
            if name == "d" and k == 1:
                found[k, 1] = lax.ppermute(found[0, 1], "sp", ring)
            else:
                found[k, 1] = lax.ppermute(found[k, 0], "sp", swap)
        return found

    small = is_small(n_sp, model)
    if small:
        gates, values, downs = (
            spread(w, name)
            for w, name in ((gate_proj, "g"), (value_proj, "v"), (down_proj, "d"))
        )
        wide, paired = nz, True
    else:
        gates, values, downs = (
            {(0, 0): lax.all_gather(w, "sp", axis=0, tiled=True)}
            for w in (gate_proj, value_proj, down_proj)
        )
        wide, paired = 1, False
    order = tuple(gates)
    mate_proj = mate(out_proj)

    half_state = ((heads, qk // 2 + 16, hv), bf16)
    stay, go = call(
        summary_kernel,
        (half_state, half_state),
        (info, key_rows, value_rows, input_gate_pre, forget_gate_pre),
        loads=True,
    )
    partner = lax.ppermute(go, "sp", swap)
    total = call(pair_kernel, half_state, (info, stay, partner))
    states = []
    reach = 1
    while reach < nz:
        route = [(i, i + 2 * reach) for i in range(n_sp - 2 * reach)]
        states.insert(0, lax.ppermute(total, "sp", route))
        reach *= 2
        if reach < nz:
            total = call(combine_kernel, half_state, (info, states[0], total))
    before, across = call(entering_kernel, (half_state, half_state), (info, stay, partner, *states))
    across = lax.ppermute(across, "sp", swap)
    inner, side = call(
        inner_kernel,
        (((rows, heads * hv), f32), ((heads, rows, 128), f32)),
        (info, query_rows, key_rows, value_rows, input_gate_pre, forget_gate_pre),
    )
    kept, sent = call(
        output_kernel,
        (((ny, step, heads * hv), bf16), ((ny, step, heads * hv), bf16)),
        (info, query_rows, out_gate_pre, inner, side, before, across),
    )
    got = mate(sent)

    parts = []
    for d in [*range(1, ny), 0]:
        part = call(
            functools.partial(project_kernel, d, ny),
            ((step, model), bf16),
            (info, kept, got, out_proj, mate_proj),
        )
        parts.append(chips(part, d) if d else part)
    stream, normed = call(
        stream_kernel,
        (((step, model), bf16), ((step, model), bf16)),
        (info, residual, mix_gain[None], pre_gain[None], *parts),
    )

    pieces = []
    for d in range(ny):
        piece = chips(normed, d) if d else normed
        pieces += [piece, mate(piece)]
    last_rows = jnp.where(tp % 2 == 1, normed[step - PAD :], pieces[1][step - PAD :])
    halos = [
        lax.ppermute(
            last_rows,
            ("sp", "tp"),
            [
                (i * n_tp + n_tp - 2 + c, (i + 1) * n_tp + 2 * j + c)
                for i in range(n_sp - 1)
                for c in range(2)
            ],
        )
        for j in range(ny)
    ]

    up_gate, group_rows = call(
        functools.partial(gate_kernel_, order, wide, paired, ny),
        (((PAD + rows, width), bf16), ((PAD + rows, model), bf16)),
        (info, *halos, *pieces, *(gates[o] for o in order)),
        scratch=(pltpu.VMEM((model // len(order), width), bf16), pltpu.SemaphoreType.DMA),
        outside=(1 + ny + n_tp,),
    )
    hidden_keep, hidden_send = call(
        functools.partial(up_kernel, order, wide, paired),
        (((ny, step, width), bf16), ((ny, step, width), bf16)),
        (info, gate_kernel, value_kernel, group_rows, up_gate, *(values[o] for o in order)),
        scratch=(pltpu.VMEM((2, PAD + rows, width), f32),),
    )
    arrival = sorted(order, key=lambda o: o[0] + o[1] * {0: 1, 1: nz + 1}.get(o[0], nz - 1))
    cuts = [len(arrival) * i // 8 for i in (0, 4, 7, 8)]
    groups = [arrival[a:b] for a, b in zip(cuts, cuts[1:]) if b > a]
    rows_of = model // len(order)
    parts = [[] for _ in groups]
    for d in [*range(1, ny), 0]:
        for g, blocks in enumerate(groups):
            shape = ((step, rows_of * len(blocks)), bf16)
            mine, away = call(
                functools.partial(down_kernel, d),
                (shape, shape),
                (info, hidden_keep, hidden_send, *(downs[o] for o in blocks)),
            )
            theirs = mate(away)
            if d:
                both = call(add_kernel, shape, (info, mine, theirs))
                route = [(i, (i + 2 * d) % n_tp) for i in range(n_tp)]
                parts[g].append(lax.ppermute(both, "tp", route))
            else:
                parts[g] += [mine, theirs]
    return call(
        functools.partial(result_kernel, groups, rows_of, wide, paired),
        ((step, model), bf16),
        (info, stream, post_gain[None], *(p for group in parts for p in group)),
        scratch=(pltpu.VMEM((step, model), f32),),
    )


def solution(mesh):
    return jax.shard_map(
        layer,
        mesh=mesh,
        in_specs=(
            P("sp", "tp"),
            P("sp", "tp"),
            P("sp", "tp"),
            P("sp", "tp"),
            P("tp", "sp"),
            P("tp", "sp"),
            P(("sp", "tp"), None),
            P("tp", None),
            P(),
            P(),
            P("sp", "tp"),
            P("sp", "tp"),
            P(None, "tp"),
            P(None, "tp"),
            P("sp", "tp"),
            P(),
        ),
        out_specs=P(("sp", "tp"), None),
        check_vma=False,
    )
```

```python
import functools

import jax
import jax.numpy as jnp
from jax import lax
from jax.experimental import pallas as pl
from jax.experimental.pallas import tpu as pltpu
from jax.sharding import PartitionSpec as P

CONV = 3
PAD = 16
gate_cap = 15.0
epsilon = 1e-06
far_below = -1e30
f32 = jnp.float32
bf16 = jnp.bfloat16


SMEM = pl.BlockSpec(memory_space=pltpu.SMEM)
VMEM = pl.BlockSpec(memory_space=pltpu.VMEM)
HBM = pl.BlockSpec(memory_space=pltpu.HBM)


def call(kernel, out, args, scratch=(), mib=16, loads=False, outside=()):
    specs = [SMEM if i == 0 else HBM if i in outside else VMEM for i in range(len(args))]
    args = [
        a
        if i == 0 or loads
        else pltpu.with_memory_space_constraint(a, pltpu.HBM if i in outside else pltpu.VMEM)
        for i, a in enumerate(args)
    ]
    many = isinstance(out[0][0], tuple)
    return pl.pallas_call(
        kernel,
        out_shape=tuple(jax.ShapeDtypeStruct(*o) for o in out)
        if many
        else jax.ShapeDtypeStruct(*out),
        in_specs=specs,
        out_specs=tuple(VMEM for _ in out) if many else VMEM,
        scratch_shapes=list(scratch),
        compiler_params=pltpu.CompilerParams(vmem_limit_bytes=mib * 2**20),
    )(*args)


def softcap(values):
    return gate_cap * jnp.tanh(values / gate_cap)


def log_gates(ig, fg):
    log_input = softcap(ig)
    capped = softcap(fg)
    log_forget = jnp.minimum(capped, 0.0) - jnp.log1p(jnp.exp(-jnp.abs(capped)))
    rows = ig.shape[1]
    lane = lax.broadcasted_iota(jnp.int32, (8, rows), 1)
    running = jnp.broadcast_to(log_forget, (8, rows))
    reach = 1
    while reach < rows:
        running = running + jnp.where(lane >= reach, pltpu.roll(running, reach, 1), 0.0)
        reach *= 2
    running = running[:1]
    return log_input, running


def column(row):
    return jnp.broadcast_to(row, (128, row.shape[1])).T[:, :1]


def store_state(ref, h, state):
    memory, normer, total, peak = state
    rows, hv = memory.shape
    side = jnp.concatenate(
        (
            normer,
            jnp.broadcast_to(total, (1, 128)),
            jnp.broadcast_to(peak, (1, hv - rows - 128)),
        ),
        axis=1,
    )
    high = side.astype(bf16).astype(f32)
    middle = (side - high).astype(bf16).astype(f32)
    low = (side - high - middle).astype(bf16).astype(f32)
    tail = jnp.concatenate((high, middle, low, jnp.zeros((13, hv), f32)), axis=0)
    ref[h, :rows, :] = memory.astype(bf16)
    ref[h, rows:, :] = tail.astype(bf16)


def load_state(ref, h):
    rows = ref.shape[1] - 16
    tail = ref[h, rows:, :].astype(f32)
    side = tail[0:1] + tail[1:2] + tail[2:3]
    return (
        ref[h, :rows, :].astype(f32),
        side[:, :rows],
        side[:, rows : rows + 1],
        side[:, rows + 128 : rows + 129],
    )


def combine(previous, following):
    prev_memory, prev_normer, prev_total, prev_peak = previous
    next_memory, next_normer, next_total, next_peak = following
    peak = jnp.maximum(next_total + prev_peak, next_peak)
    prev_scale = jnp.exp(next_total + prev_peak - peak)
    next_scale = jnp.exp(next_peak - peak)
    return (
        prev_scale * prev_memory + next_scale * next_memory,
        prev_scale * prev_normer + next_scale * next_normer,
        prev_total + next_total,
        peak,
    )


def summary_kernel(info, key, value, ig, fg, stay, go):
    heads = ig.shape[0]
    qk = key.shape[1] // heads
    hv = value.shape[1] // heads
    for h in range(heads):
        log_input, running = log_gates(ig[h : h + 1, :], fg[h : h + 1, :])
        total = running[:, -1:]
        lead = total - running + log_input
        peak = jnp.max(lead, axis=1, keepdims=True)
        weights = column(jnp.exp(lead - peak))
        weighted = key[:, h * qk : (h + 1) * qk].astype(f32) * weights
        memory = lax.dot_general(
            weighted.astype(bf16),
            value[:, h * hv : (h + 1) * hv],
            (((0,), (0,)), ((), ())),
            preferred_element_type=f32,
        )
        normer = jnp.sum(weighted, axis=0, keepdims=True)
        half = qk // 2
        halves = [
            (memory[:half], normer[:, :half], total, peak),
            (memory[half:], normer[:, half:], total, peak),
        ]
        for parity in range(2):

            @pl.when(info[1] == parity)
            def _():
                store_state(stay, h, halves[parity])
                store_state(go, h, halves[1 - parity])


def inner_kernel(info, query, key, value, ig, fg, numerator, side):
    heads = ig.shape[0]
    qk = key.shape[1] // heads
    hv = value.shape[1] // heads
    rows = key.shape[0]
    for h in range(heads):
        log_input, running = log_gates(ig[h : h + 1, :], fg[h : h + 1, :])
        running_column = column(running)
        causal = lax.broadcasted_iota(jnp.int32, (rows, rows), 0) >= lax.broadcasted_iota(
            jnp.int32, (rows, rows), 1
        )
        logs = jnp.where(causal, running_column - running + log_input, far_below)
        peak = jnp.max(logs, axis=1, keepdims=True)
        scores = lax.dot_general(
            query[:, h * qk : (h + 1) * qk] * bf16(qk**-0.5),
            key[:, h * qk : (h + 1) * qk],
            (((1,), (1,)), ((), ())),
            preferred_element_type=f32,
        ) * jnp.exp(logs - peak)
        numerator[:, h * hv : (h + 1) * hv] = jnp.dot(
            scores.astype(bf16), value[:, h * hv : (h + 1) * hv], preferred_element_type=f32
        )
        lane = lax.broadcasted_iota(jnp.int32, (rows, 128), 1)
        total = jnp.sum(scores, axis=1, keepdims=True)
        side[h] = jnp.where(lane == 0, total, jnp.where(lane == 1, peak, running_column))


def pair_kernel(info, mine, theirs, out):
    first = info[1] == 0
    for h in range(mine.shape[0]):
        own = load_state(mine, h)
        other = load_state(theirs, h)
        previous = tuple(jnp.where(first, a, b) for a, b in zip(own, other))
        following = tuple(jnp.where(first, b, a) for a, b in zip(own, other))
        store_state(out, h, combine(previous, following))


def combine_kernel(info, earlier, later, out):
    for h in range(earlier.shape[0]):
        store_state(out, h, combine(load_state(earlier, h), load_state(later, h)))


def entering_kernel(info, mine, theirs, *refs):
    states, keep, send = refs[:-2], refs[-2], refs[-1]
    first = info[1] == 0
    for h in range(mine.shape[0]):
        opening = tuple(
            jnp.where(first, a, b) for a, b in zip(load_state(mine, h), load_state(theirs, h))
        )
        before = None
        for ref in states:
            state = load_state(ref, h)
            before = state if before is None else combine(before, state)
        if before is None:
            before = tuple(jnp.zeros_like(a) for a in opening)
        after = combine(before, opening)
        store_state(keep, h, tuple(jnp.where(first, a, b) for a, b in zip(before, after)))
        store_state(send, h, tuple(jnp.where(first, b, a) for a, b in zip(before, after)))


def output_kernel(info, query, out_gate, numerator, side, mine, theirs, keep, send):
    heads = side.shape[0]
    qk = query.shape[1] // heads
    hv = out_gate.shape[1] // heads
    half = qk // 2
    blocks = 2 * keep.shape[0]
    step = keep.shape[1]
    for h in range(heads):
        own_half = pl.multiple_of(h * qk + info[1] * half, half)
        other_half = pl.multiple_of(h * qk + (1 - info[1]) * half, half)
        own_query = query[:, pl.ds(own_half, half)] * bf16(qk**-0.5)
        other_query = query[:, pl.ds(other_half, half)] * bf16(qk**-0.5)
        _, own_normer, _, before = load_state(mine, h)
        _, other_normer, _, _ = load_state(theirs, h)
        top = jnp.dot(own_query, mine[h, :half, :], preferred_element_type=f32) + jnp.dot(
            other_query, theirs[h, :half, :], preferred_element_type=f32
        )
        bottom = jnp.sum(
            own_query.astype(f32) * own_normer + other_query.astype(f32) * other_normer,
            axis=1,
            keepdims=True,
        )
        inner_total = side[h, :, 0:1]
        inner_peak = side[h, :, 1:2]
        carried = side[h, :, 2:3] + before
        peak = jnp.maximum(carried, inner_peak)
        outer = jnp.exp(carried - peak)
        inner = jnp.exp(inner_peak - peak)
        denominator = outer * bottom + inner * inner_total
        scale = 1.0 / jnp.maximum(jnp.abs(denominator), jnp.exp(-peak))
        cell = (outer * top + inner * numerator[:, h * hv : (h + 1) * hv]) * scale
        opened = cell * jax.nn.sigmoid(out_gate[:, h * hv : (h + 1) * hv].astype(f32))
        gated = opened.astype(bf16)
        for parity in range(2):

            @pl.when(info[3] == parity)
            def _():
                for j in range(blocks):
                    ref = keep if j % 2 == parity else send
                    ref[j // 2, :, h * hv : (h + 1) * hv] = gated[j * step : (j + 1) * step]


def project_kernel(shift, count, info, kept, got, own_weight, mate_weight, out):
    block = lax.rem(info[2] + shift, count)
    out[...] = (
        jnp.dot(kept[block], own_weight[...], preferred_element_type=f32)
        + jnp.dot(got[block], mate_weight[...], preferred_element_type=f32)
    ).astype(bf16)


def normalize(values, gains):
    return values * lax.rsqrt(jnp.mean(values * values, axis=-1, keepdims=True) + epsilon) * gains


def stream_kernel(info, residual, mix_gain, pre_gain, *refs):
    parts, stream_out, normed_out = refs[:-2], refs[-2], refs[-1]
    summed = parts[0][...].astype(f32)
    for part in parts[1:]:
        summed = summed + part[...].astype(f32)
    mixed = summed.astype(bf16).astype(f32)
    stream = (residual[...].astype(f32) + normalize(mixed, mix_gain[...])).astype(bf16)
    stream_out[...] = stream
    normed_out[...] = normalize(stream.astype(f32), pre_gain[...]).astype(bf16)


def chunk_of(info, k, e, nz, pair):
    z = lax.rem(info[0] - k + nz, nz)
    return z * 2 + jnp.bitwise_xor(info[1], e) if pair else z


def tiles_of(width):
    tile = 256 if width % 256 == 0 else width
    return [slice(t, t + tile) for t in range(0, width, tile)]


def times_weight(order, nz, pair, info, rows_all, blocks, span):
    rows = blocks[0].shape[0]
    product = None
    for (k, e), block in zip(order, blocks):
        start = pl.multiple_of(chunk_of(info, k, e, nz, pair) * rows, min(rows, 128))
        term = jnp.dot(
            rows_all[:, pl.ds(start, rows)], block[:, span], preferred_element_type=f32
        )
        product = term if product is None else product + term
    return product.astype(bf16)


def gate_kernel_(order, nz, pair, ny, info, *refs):
    halos = refs[:ny]
    pieces = refs[ny : 3 * ny]
    blocks = refs[3 * ny : 3 * ny + len(order)]
    out, rows_all, own, sem = refs[3 * ny + len(order) :]
    copy = pltpu.make_async_copy(blocks[0], own, sem)
    copy.start()
    blocks = (*blocks[1:], own)
    order = (*order[1:], order[0])
    halo = halos[0][...]
    for ref in halos[1:]:
        halo = halo + ref[...]
    rows_all[0:PAD, :] = halo
    step = pieces[0].shape[0]
    for i, piece in enumerate(pieces):
        d, other = i // 2, i % 2
        chip = lax.rem(info[2] - d + ny, ny)
        core = 1 - info[3] if other else info[3]
        start = pl.multiple_of(PAD + (chip * 2 + core) * step, 16)
        rows_all[pl.ds(start, step), :] = piece[...]
    copy.wait()
    for span in tiles_of(out.shape[1]):
        out[:, span] = times_weight(order, nz, pair, info, rows_all, blocks, span)


def up_kernel(order, nz, pair, info, gate_taps, value_taps, rows_all, gates, *refs):
    blocks = refs[: len(order)]
    keep, send, up = refs[len(order) :]
    ny, step, width = keep.shape
    total = 2 * ny * step
    up[0] = gates[...].astype(f32)
    for span in tiles_of(width):
        up[1, :, span] = times_weight(order, nz, pair, info, rows_all, blocks, span).astype(f32)
        summed = []
        for g, taps in enumerate((gate_taps, value_taps)):
            first = PAD - CONV + 1
            conv = taps[0:1, span] * up[g, first : first + total, span]
            for j in range(1, CONV):
                conv = conv + taps[j : j + 1, span] * up[g, first + j : first + j + total, span]
            summed.append(conv)
        hidden = (summed[0] / (1.0 + jnp.exp(-summed[0])) * summed[1]).astype(bf16)
        for parity in range(2):

            @pl.when(info[3] == parity)
            def _():
                for j in range(2 * ny):
                    ref = keep if j % 2 == parity else send
                    ref[j // 2, :, span] = hidden[j * step : (j + 1) * step]


def down_kernel(shift, info, keep, send, *refs):
    blocks, keep_out, send_out = refs[:-2], refs[-2], refs[-1]
    chip = lax.rem(info[2] + shift, keep.shape[0])
    step = keep.shape[1]
    both = jnp.concatenate((keep[chip], send[chip]), axis=0)
    start = 0
    for block in blocks:
        end = start + block.shape[0]
        product = lax.dot_general(
            both, block[...], (((1,), (1,)), ((), ())), preferred_element_type=f32
        ).astype(bf16)
        keep_out[:, start:end] = product[:step]
        send_out[:, start:end] = product[step:]
        start = end


def add_kernel(info, mine, theirs, out):
    out[...] = (mine[...].astype(f32) + theirs[...].astype(f32)).astype(bf16)


def result_kernel(groups, counts, rows, nz, pair, info, stream, post_gain, *refs):
    out, summed = refs[-2], refs[-1]
    for g, order in enumerate(groups):
        parts = refs[sum(counts[:g]) : sum(counts[: g + 1])]
        total = parts[0][...].astype(f32)
        for part in parts[1:]:
            total = total + part[...].astype(f32)
        for i, (k, e) in enumerate(order):
            start = pl.multiple_of(chunk_of(info, k, e, nz, pair) * rows, min(rows, 128))
            summed[:, pl.ds(start, rows)] = total[:, i * rows : (i + 1) * rows]
    ffn = summed[...].astype(bf16).astype(f32)
    out[...] = (stream[...].astype(f32) + normalize(ffn, post_gain[...])).astype(bf16)


def is_small(n_sp, model):
    return n_sp <= 16 and model // n_sp % 128 == 0


def layer(
    query_rows,
    key_rows,
    value_rows,
    out_gate_pre,
    input_gate_pre,
    forget_gate_pre,
    residual,
    out_proj,
    mix_gain,
    pre_gain,
    gate_proj,
    value_proj,
    gate_kernel,
    value_kernel,
    down_proj,
    post_gain,
):
    n_sp = lax.axis_size("sp")
    n_tp = lax.axis_size("tp")
    nz = n_sp // 2
    ny = n_tp // 2
    rows, width = query_rows.shape[0], gate_proj.shape[1]
    heads = input_gate_pre.shape[0]
    qk = query_rows.shape[1] // heads
    hv = value_rows.shape[1] // heads
    model = residual.shape[1]
    step = rows // n_tp

    sp = lax.axis_index("sp")
    tp = lax.axis_index("tp")
    z, x = sp // 2, sp % 2
    lane = lax.iota(jnp.int32, 8)
    info = jnp.where(
        lane == 0, z, jnp.where(lane == 1, x, jnp.where(lane == 2, tp // 2, tp % 2))
    ).astype(jnp.int32)

    ring = [(i, (i + 2) % n_sp) for i in range(n_sp)]
    swap = [(i, i ^ 1) for i in range(n_sp)]

    mate = lambda a: lax.ppermute(a, "tp", [(i, i ^ 1) for i in range(n_tp)])
    chips = lambda a, d: lax.ppermute(a, "tp", [(i, (i + 2 * d) % n_tp) for i in range(n_tp)])

    def spread(block, name):
        found = {(0, 0): block}
        for k in range(nz):
            if k:
                found[k, 0] = lax.ppermute(found[k - 1, 0], "sp", ring)
            if name == "d" and k == 1:
                found[k, 1] = lax.ppermute(found[0, 1], "sp", ring)
            else:
                found[k, 1] = lax.ppermute(found[k, 0], "sp", swap)
        return found

    small = is_small(n_sp, model)
    if small:
        gates, values, downs = (
            spread(w, name)
            for w, name in ((gate_proj, "g"), (value_proj, "v"), (down_proj, "d"))
        )
        wide, paired = nz, True
    else:
        gates, values, downs = (
            {(0, 0): lax.all_gather(w, "sp", axis=0, tiled=True)}
            for w in (gate_proj, value_proj, down_proj)
        )
        wide, paired = 1, False
    order = tuple(gates)
    mate_proj = mate(out_proj)

    half_state = ((heads, qk // 2 + 16, hv), bf16)
    stay, go = call(
        summary_kernel,
        (half_state, half_state),
        (info, key_rows, value_rows, input_gate_pre, forget_gate_pre),
        loads=True,
    )
    partner = lax.ppermute(go, "sp", swap)
    total = call(pair_kernel, half_state, (info, stay, partner))
    states = []
    reach = 1
    while reach < nz:
        route = [(i, i + 2 * reach) for i in range(n_sp - 2 * reach)]
        states.insert(0, lax.ppermute(total, "sp", route))
        reach *= 2
        if reach < nz:
            total = call(combine_kernel, half_state, (info, states[0], total))
    before, across = call(entering_kernel, (half_state, half_state), (info, stay, partner, *states))
    across = lax.ppermute(across, "sp", swap)
    inner, side = call(
        inner_kernel,
        (((rows, heads * hv), f32), ((heads, rows, 128), f32)),
        (info, query_rows, key_rows, value_rows, input_gate_pre, forget_gate_pre),
    )
    kept, sent = call(
        output_kernel,
        (((ny, step, heads * hv), bf16), ((ny, step, heads * hv), bf16)),
        (info, query_rows, out_gate_pre, inner, side, before, across),
    )
    got = mate(sent)

    parts = []
    for d in [*range(1, ny), 0]:
        part = call(
            functools.partial(project_kernel, d, ny),
            ((step, model), bf16),
            (info, kept, got, out_proj, mate_proj),
        )
        parts.append(chips(part, d) if d else part)
    stream, normed = call(
        stream_kernel,
        (((step, model), bf16), ((step, model), bf16)),
        (info, residual, mix_gain[None], pre_gain[None], *parts),
    )

    pieces = []
    for d in range(ny):
        piece = chips(normed, d) if d else normed
        pieces += [piece, mate(piece)]
    last_rows = jnp.where(tp % 2 == 1, normed[step - PAD :], pieces[1][step - PAD :])
    halos = [
        lax.ppermute(
            last_rows,
            ("sp", "tp"),
            [
                (i * n_tp + n_tp - 2 + c, (i + 1) * n_tp + 2 * j + c)
                for i in range(n_sp - 1)
                for c in range(2)
            ],
        )
        for j in range(ny)
    ]

    up_gate, group_rows = call(
        functools.partial(gate_kernel_, order, wide, paired, ny),
        (((PAD + rows, width), bf16), ((PAD + rows, model), bf16)),
        (info, *halos, *pieces, *(gates[o] for o in order)),
        scratch=(pltpu.VMEM((model // len(order), width), bf16), pltpu.SemaphoreType.DMA),
        outside=(1 + ny + n_tp,),
    )
    hidden_keep, hidden_send = call(
        functools.partial(up_kernel, order, wide, paired),
        (((ny, step, width), bf16), ((ny, step, width), bf16)),
        (info, gate_kernel, value_kernel, group_rows, up_gate, *(values[o] for o in order)),
        scratch=(pltpu.VMEM((2, PAD + rows, width), f32),),
    )
    arrival = sorted(order, key=lambda o: o[0] + o[1] * {0: 1, 1: nz + 1}.get(o[0], nz - 1))
    cuts = [len(arrival) * i // 8 for i in (0, 4, 7, 8)]
    groups = [arrival[a:b] for a, b in zip(cuts, cuts[1:]) if b > a]
    rows_of = model // len(order)
    parts = [[] for _ in groups]
    for d in [*range(1, ny), 0]:
        for g, blocks in enumerate(groups):
            shape = ((step, rows_of * len(blocks)), bf16)
            mine, away = call(
                functools.partial(down_kernel, d),
                (shape, shape),
                (info, hidden_keep, hidden_send, *(downs[o] for o in blocks)),
            )
            straight = [(i, (i + 2 * d) % n_tp) for i in range(n_tp)]
            crossed = [(i, ((i + 2 * d) % n_tp) ^ 1) for i in range(n_tp)]
            if d and g and g == len(groups) - 1:
                parts[g].append(lax.ppermute(mine, "tp", straight))
                parts[g].append(lax.ppermute(away, "tp", crossed))
                continue
            theirs = mate(away)
            if d:
                both = call(add_kernel, shape, (info, mine, theirs))
                parts[g].append(lax.ppermute(both, "tp", straight))
            else:
                parts[g] += [mine, theirs]
    return call(
        functools.partial(
            result_kernel, groups, [len(p) for p in parts], rows_of, wide, paired
        ),
        ((step, model), bf16),
        (info, stream, post_gain[None], *(p for group in parts for p in group)),
        scratch=(pltpu.VMEM((step, model), f32),),
    )


def solution(mesh):
    return jax.shard_map(
        layer,
        mesh=mesh,
        in_specs=(
            P("sp", "tp"),
            P("sp", "tp"),
            P("sp", "tp"),
            P("sp", "tp"),
            P("tp", "sp"),
            P("tp", "sp"),
            P(("sp", "tp"), None),
            P("tp", None),
            P(),
            P(),
            P("sp", "tp"),
            P("sp", "tp"),
            P(None, "tp"),
            P(None, "tp"),
            P("sp", "tp"),
            P(),
        ),
        out_specs=P(("sp", "tp"), None),
        check_vma=False,
    )
```
